32 devices in a mesh: ep: 8 (over z, x), tp: 4 (over y, core).
Axes of the slice: x: 2, y: 2, z: 4, core: 2. Of those that a mesh axis runs over, the one named last changes fastest.
Arguments:
- tokens: bfloat16 [512, 2048], P('ep', 'tp')
- norm_gain: float32 [2048], P('tp'), may hold values from 0.1 to 1.9
- expert_ids: int32 [512, 4], P('ep'), may hold values from 0 to 7, all different within a row; in each aligned block of 64 rows (0 to 63, 64 to 127, ...) at most 64 rows name the same one
- route_weights: float32 [512, 4], P('ep'), may hold values from 0.1 to 1
- gate_proj: bfloat16 [8, 2048, 2048], P('ep', None, 'tp'), may hold values from -0.5 to 0.5
- up_proj: bfloat16 [8, 2048, 2048], P('ep', None, 'tp'), may hold values from -0.5 to 0.5
- down_proj: bfloat16 [8, 2048, 2048], P('ep', 'tp')
- final_gain: float32 [2048], P('tp'), may hold values from 0.1 to 1.9
Outputs:
- layer_output: bfloat16 [512, 2048], P('ep', 'tp')
The draws below stay inside these ranges and needn't reach their ends.
Inputs may be any that keep to these rules, and one draw needn't show every extreme that they name: `expert_ids`: each row names 4 different experts. Within the 64 rows of one device no expert is named by more than 64 rows, a bound that some block reaches.
All inputs are finite; a program needn't handle non-finite values.
Results may differ from the reference program's by a relative error of at most 0.017.
Values may be sent and summed in bfloat16 or wider, within the bound.
A program may use at most 64 MiB of HBM per device.

```python
import math
import jax
import jax.numpy as jnp
import numpy as np
from jax import lax

D = 2048
FF = 2048
TOP_K = 4
TOK_DEV = 64
EXPERTS = 8
TOKENS = 512
CAP = 64
N_EP = 8
N_TP = 4


def column_rise(count):
    return jnp.exp(math.log(6.0) * jnp.arange(count, dtype=jnp.float32) / (count - 1))


def draw_tokens(key, part):
    first_key, second_key = jax.random.split(key, 2)
    row_scales = jnp.exp(jax.random.uniform(second_key, (TOKENS, 1), jnp.float32, minval=math.log(0.3), maxval=math.log(3.0)))
    base = jax.random.normal(first_key, (TOKENS, D), jnp.float32)
    return (base * row_scales * column_rise(D)[None, :]).astype(jnp.bfloat16)


def draw_down_proj(key, part):
    first_key = jax.random.fold_in(key, 0)
    base = jax.random.normal(first_key, (EXPERTS, FF, D), jnp.float32)
    return (base * FF ** (-0.5) * column_rise(D)[None, None, :]).astype(jnp.bfloat16)


def shard_levels(key, extent, shards, low, top_value):
    def one(axis_at, blocks):
        steps = jax.random.uniform(jax.random.fold_in(jax.random.fold_in(key, 6), axis_at), (blocks,), jnp.float32, low / len(shards), top_value / len(shards))
        return jnp.repeat(jnp.exp(steps), extent[axis_at] // blocks).reshape((-1,) + (1,) * (len(extent) - axis_at - 1))

    gain = one(*shards[0])
    for cut in shards[1:]:
        gain = gain * one(*cut)
    return gain


def assign_block(own_key, own, number, rows, amount, top, most, skew):
    ranking = jax.random.permutation(own_key, amount)
    packed, ordinary = portions_of(amount, rows * top, most, skew, True), portions_of(amount, rows * top, most, skew, False)
    places = jnp.arange(amount)

    def named(lengths, turn):
        used = int((lengths > 0).sum())
        fixed = max(1, used // 4)
        moved = fixed + (places - fixed + turn * (used - fixed)) % max(1, amount - fixed)
        return jnp.zeros((amount,), jnp.int32).at[ranking[jnp.where(places < fixed, places, moved)]].set(jnp.asarray(lengths, jnp.int32))

    lengths = jnp.where(number % 4 == 0, named(packed, number // 4), named(ordinary, number - number // 4 - 1))
    mixed = jax.random.permutation(jax.random.fold_in(own, 3), amount)
    giver, sink = mixed[0:amount // 2 * 2:2], mixed[1:amount // 2 * 2:2]
    margin = jnp.minimum(lengths[giver] - 1, most - lengths[sink]) // 2
    margin = jnp.where((giver == ranking[0]) | (sink == ranking[0]) | (lengths[sink] == 0), 0, jnp.maximum(margin, 0))
    moved = jax.random.randint(jax.random.fold_in(own, 4), (amount // 2,), 0, 1 << 20) % (margin + 1)
    lengths = lengths.at[giver].add(-moved).at[sink].add(moved)
    labels = jnp.searchsorted(jnp.cumsum(lengths), jnp.arange(rows * top), side="right").astype(jnp.int32)
    table = labels.reshape(top, rows).T
    table = table[jax.random.permutation(jax.random.fold_in(own, 1), rows)]
    turn = jax.random.randint(jax.random.fold_in(own, 2), (rows, 1), 0, top)
    return jnp.take_along_axis(table, (jnp.arange(top)[None, :] + turn) % top, axis=1)


def portions_of(number_of, total, limit, skew, full):
    portions = [(1 << 20) // math.isqrt(rank ** skew) + 1 for rank in range(1, number_of + 1)]
    largest = limit if full else min(limit, max(-(-total // number_of), total * portions[0] // sum(portions)))
    least = 1 if total - largest >= number_of - 1 else 0
    counts, spare = [largest] + [least] * (number_of - 1), total - largest - least * (number_of - 1)
    while spare > 0:
        candidates = [i for i in range(1, number_of) if counts[i] < largest] or [i for i in range(1, number_of) if counts[i] < limit]
        pool, budget = sum([portions[i] for i in candidates]), spare
        for i in candidates:
            more = min(limit - counts[i], max(1, budget * portions[i] // pool), spare)
            counts[i] = counts[i] + more
            spare = spare - more
    return np.array(counts)


def normal_values(own_key, shape, scale, limit, cuts=(), kind=jnp.bfloat16):
    result = scale * jax.random.normal(own_key, shape, jnp.float32)
    if cuts:
        result = result * shard_levels(own_key, shape, cuts, -0.22, 0.18)
    return jnp.clip(result, -limit, limit).astype(kind)


def setup_inputs(seed: int = 0) -> dict:
    splits = jax.random.split(jax.random.key(seed), 9)
    tokens = draw_tokens(jax.random.fold_in(splits[8], 71), 0)
    norm_gain = jnp.clip(1.0 + 0.18 * jax.random.normal(splits[1], (D,), jnp.float32), 0.1, 1.9)
    expert_ids_keys = jax.random.split(jax.random.fold_in(splits[2], 1), TOKENS // TOK_DEV)
    expert_ids_turns = jax.random.permutation(jax.random.fold_in(splits[2], 3), TOKENS // TOK_DEV)
    expert_ids = jax.vmap(lambda own, number: assign_block(jax.random.fold_in(splits[2], 2), own, number, TOK_DEV, EXPERTS, TOP_K, CAP, 2))(expert_ids_keys, expert_ids_turns).reshape((TOKENS, TOP_K))
    route_weights = jnp.clip(0.1 + 0.9 * jax.random.uniform(splits[3], (TOKENS, TOP_K), jnp.float32) ** shard_levels(splits[3], (TOKENS, TOP_K), ((0, 8),), -0.2, 0.2), 0.1, 1.0)
    gate_proj = normal_values(splits[4], (EXPERTS, D, FF), (D // 16) ** -0.5, 0.5, ((0, 8), (2, 4)))
    up_proj = normal_values(splits[5], (EXPERTS, D, FF), (D // 16) ** -0.5, 0.5, ((0, 8), (2, 4)))
    down_proj = draw_down_proj(jax.random.fold_in(splits[8], 71), 0)
    final_gain = jnp.clip(1.0 + 0.18 * jax.random.normal(splits[7], (D,), jnp.float32), 0.1, 1.9)
    return {"tokens": tokens, "norm_gain": norm_gain, "expert_ids": expert_ids, "route_weights": route_weights, "gate_proj": gate_proj, "up_proj": up_proj, "down_proj": down_proj, "final_gain": final_gain}


EPSILON = 1e-05
CLAMP_LIMIT = 7.0
SIGMOID_SLOPE = 1.702

def slot_tables(id_block, gate_block, targets, capacity):
    matches = (id_block[:, :, None] == targets[None, None, :]).astype(jnp.int32)
    per_token = lax.optimization_barrier(jnp.sum(matches, axis=1))
    earlier = jnp.cumsum(per_token, axis=0) - per_token
    slot_places = lax.broadcasted_iota(jnp.int32, (1, 1, capacity), 2)
    selector = (per_token[:, :, None] * (earlier[:, :, None] == slot_places).astype(jnp.int32)).astype(jnp.float32)
    weights = lax.optimization_barrier(jnp.sum(gate_block[:, :, None] * matches.astype(jnp.float32), axis=1))
    return (selector, weights)

def reference(tokens, norm_gain, expert_ids, route_weights, gate_proj, up_proj, down_proj, final_gain):
    input_rows = tokens.astype(jnp.float32)
    row_scale = lax.rsqrt(lax.optimization_barrier(jnp.mean(input_rows * input_rows, axis=1, keepdims=True)) + EPSILON)
    normed = (input_rows * row_scale * norm_gain[None, :]).astype(jnp.bfloat16)
    targets = jnp.arange(EXPERTS, dtype=jnp.int32)

    def per_source(id_block, gate_block):
        return slot_tables(id_block, gate_block, targets, CAP)
    selector, weights = jax.vmap(per_source)(expert_ids.reshape(N_EP, TOK_DEV, TOP_K), route_weights.reshape(N_EP, TOK_DEV, TOP_K))
    blocks = normed.reshape(N_EP, TOK_DEV, D).astype(jnp.float32)
    select_by_expert = jnp.moveaxis(selector, 2, 0)
    weight_by_expert = jnp.moveaxis(weights, 2, 0)

    def one_expert(carry, inputs):
        chosen, gate_share, gate_w, up_w, down_w = inputs
        expert_rows = jnp.einsum('stc,std->scd', chosen, blocks).astype(jnp.bfloat16).reshape(-1, D)
        gate_pre = jnp.minimum(jnp.dot(expert_rows, gate_w, preferred_element_type=jnp.float32), CLAMP_LIMIT)
        up_pre = jnp.clip(jnp.dot(expert_rows, up_w, preferred_element_type=jnp.float32), -CLAMP_LIMIT, CLAMP_LIMIT)
        activated = ((up_pre + 1.0) * gate_pre * jax.nn.sigmoid(SIGMOID_SLOPE * gate_pre)).astype(jnp.bfloat16)
        partials = jnp.einsum('npf,pfd->npd', activated.reshape(-1, N_TP, FF // N_TP).astype(jnp.float32), down_w.reshape(N_TP, FF // N_TP, D).astype(jnp.float32))
        rounded = lax.optimization_barrier(partials.astype(jnp.bfloat16))
        expert_out = lax.optimization_barrier(jnp.sum(rounded.astype(jnp.float32), axis=1)).astype(jnp.bfloat16)
        contrib = jnp.einsum('stc,scd->std', chosen * gate_share[:, :, None], expert_out.astype(jnp.float32).reshape(N_EP, CAP, D))
        return (carry + contrib, None)
    summed, _ = lax.scan(one_expert, jnp.zeros((N_EP, TOK_DEV, D), jnp.float32), (select_by_expert, weight_by_expert, gate_proj, up_proj, down_proj))
    mixture = summed.reshape(TOKENS, D)
    out_scale = lax.rsqrt(lax.optimization_barrier(jnp.mean(mixture * mixture, axis=1, keepdims=True)) + EPSILON)
    return (mixture * out_scale * final_gain[None, :]).astype(jnp.bfloat16)
```

```python
import functools

import jax
import jax.numpy as jnp
from jax import lax
from jax.experimental import pallas as pl
from jax.experimental.pallas import tpu as pltpu
from jax.sharding import PartitionSpec as P

EPSILON = 1e-05
CLAMP_LIMIT = 7.0
MESH = pl.DeviceIdType.MESH
PER_GROUP = 17
SIGMOID_SLOPE = 1.702


def slot_tables(id_block, gate_block, targets, capacity):
    matches = (id_block[:, :, None] == targets[None, None, :]).astype(jnp.int32)
    per_token = jnp.sum(matches, axis=1)
    earlier = jnp.cumsum(per_token, axis=0) - per_token
    slot_places = lax.broadcasted_iota(jnp.int32, (1, 1, capacity), 2)
    selector = (
        per_token[:, :, None] * (earlier[:, :, None] == slot_places).astype(jnp.int32)
    ).astype(jnp.float32)
    weights = jnp.sum(gate_block[:, :, None] * matches.astype(jnp.float32), axis=1)
    return (selector, weights)


def expert_partial(flat_rows, gate_proj, up_proj, down_proj):
    gate_pre = jnp.minimum(
        jnp.dot(flat_rows, gate_proj[0], preferred_element_type=jnp.float32), CLAMP_LIMIT
    )
    up_pre = jnp.clip(
        jnp.dot(flat_rows, up_proj[0], preferred_element_type=jnp.float32),
        -CLAMP_LIMIT,
        CLAMP_LIMIT,
    )
    activated = ((up_pre + 1.0) * gate_pre * jax.nn.sigmoid(SIGMOID_SLOPE * gate_pre)).astype(
        jnp.bfloat16
    )
    return jnp.dot(activated, down_proj[0], preferred_element_type=jnp.float32)


def local(tokens, norm_gain, expert_ids, route_weights, gate_proj, up_proj, down_proj, final_gain):
    tok_rows, local_width = tokens.shape
    choose_count = expert_ids.shape[1]
    model_width = local_width * lax.axis_size("tp")
    expert_count = lax.axis_size("ep")
    capacity = min(tok_rows, 2 * tok_rows * choose_count // expert_count)
    input_rows = tokens.astype(jnp.float32)
    squares = lax.psum(jnp.sum(input_rows * input_rows, axis=1), "tp")
    normed = (
        input_rows * lax.rsqrt(squares / model_width + EPSILON)[:, None] * norm_gain[None, :]
    ).astype(jnp.bfloat16)
    targets = lax.iota(jnp.int32, expert_count)
    selector, weights = slot_tables(expert_ids, route_weights, targets, capacity)
    picker = selector.astype(jnp.bfloat16)
    outbound = jnp.einsum("tec,td->ecd", picker, normed, preferred_element_type=jnp.float32).astype(
        jnp.bfloat16
    )
    received = lax.all_gather(
        lax.all_to_all(outbound, "ep", split_axis=0, concat_axis=0, tiled=True),
        "tp",
        axis=2,
        tiled=True,
    )
    flat_rows = received.reshape(-1, model_width)
    partial_value = expert_partial(flat_rows, gate_proj, up_proj, down_proj)
    summed = lax.psum_scatter(
        partial_value.astype(jnp.bfloat16), "tp", scatter_dimension=1, tiled=True
    )
    expert_out = summed.reshape(received.shape[0], received.shape[1], local_width)
    returned = lax.all_to_all(expert_out, "ep", split_axis=0, concat_axis=0, tiled=True)
    mixture = jnp.einsum(
        "tec,ecd->td", selector * weights[:, :, None], returned.astype(jnp.float32)
    )
    squares_out = lax.psum(jnp.sum(mixture * mixture, axis=1), "tp")
    return (
        mixture * lax.rsqrt(squares_out / model_width + EPSILON)[:, None] * final_gain[None, :]
    ).astype(jnp.bfloat16)


def fused_kernel(
    ep_size,
    tokens,
    norm_gain,
    expert_ids,
    route_weights,
    gate_hbm,
    up_hbm,
    down_hbm,
    final_gain,
    out,
    rows_all,
    gate_w,
    up_w,
    down_w,
    normed,
    gains,
    table,
    tables,
    own,
    pair_out,
    pair_in,
    diag_out,
    x_out,
    y_out,
    z_out,
    diag_x,
    diag_y,
    x_in,
    y_in,
    z_in,
    home,
    square_out,
    squares_in,
    weight_sem,
    send_sem,
    recv_sem,
):
    groups = ep_size // 2
    tok, width = tokens.shape
    half = tok // 2
    model_width = 4 * width
    e, t = lax.axis_index("ep"), lax.axis_index("tp")
    z, x, y, c = e // 2, e % 2, t // 2, t % 2

    def device(zz, xx, yy, cc):
        return (zz * 2 + xx, yy * 2 + cc)

    x_peer, y_peer, c_peer = device(z, 1 - x, y, c), device(z, x, 1 - y, c), device(z, x, y, 1 - c)
    tp_peers = {(1, 0): y_peer, (0, 1): c_peer, (1, 1): device(z, x, 1 - y, 1 - c)}
    ep_peers = {
        (dz, dx): device((z + dz) % groups, (x + dx) % 2, y, c)
        for dz in range(groups)
        for dx in range(2)
        if dz or dx
    }

    loads = [
        pltpu.make_async_copy(src.at[0], dst, weight_sem.at[i])
        for i, (src, dst) in enumerate(((gate_hbm, gate_w), (up_hbm, up_w), (down_hbm, down_w)))
    ]
    for load in loads:
        load.start()

    barrier = pltpu.get_barrier_semaphore()
    peers = list(tp_peers.values()) + list(ep_peers.values())
    for peer in peers:
        pl.semaphore_signal(barrier, inc=1, device_id=peer, device_id_type=MESH)

    lanes = lax.broadcasted_iota(jnp.int32, (tok, 128), 1)
    dense = jnp.zeros((tok, 128), jnp.float32)
    for k in range(expert_ids.shape[1]):
        dense = dense + jnp.where(
            expert_ids[:, k : k + 1] == lanes, route_weights[:, k : k + 1], 0.0
        )
    table[...] = jnp.transpose(dense)[:ep_size]
    tables[e] = table[...]
    gains[t] = norm_gain[...]
    rows_all[z, t, x] = tokens[...]
    pl.semaphore_wait(barrier, len(peers))

    sent = []

    def remote(src, dst, slot, peer):
        return pltpu.make_async_remote_copy(
            src_ref=src,
            dst_ref=dst,
            send_sem=send_sem.at[slot],
            recv_sem=recv_sem.at[slot],
            device_id=peer,
            device_id_type=MESH,
        )

    def send(src, dst, slot, peer):
        copy = remote(src, dst, slot, peer)
        copy.start()
        sent.append(copy)

    def arrived(dst, slot):
        remote(dst, dst, slot, c_peer).wait_recv()

    def block(g, xx, yy, cc):
        return rows_all.at[(z + g) % groups, yy * 2 + cc, xx]

    small = groups * PER_GROUP

    def gather_z(g):
        if g:
            arrived(block(g, x, y, c), g * PER_GROUP)
        src = block(g, x, y, c) if g else tokens
        dst = block(g, x, y, c)
        send(src, dst, g * PER_GROUP + 1, x_peer)
        send(src, dst, g * PER_GROUP + 2, y_peer)
        send(src, dst, g * PER_GROUP + 3, c_peer)

    def gather_xy(g):
        base = g * PER_GROUP
        from_x = block(g, 1 - x, y, c)
        arrived(from_x, base + 1)
        send(from_x.at[pl.ds(0, half)], from_x.at[pl.ds(0, half)], base + 7, y_peer)
        send(from_x, from_x, base + 4, c_peer)
        from_y = block(g, x, 1 - y, c)
        arrived(from_y, base + 2)
        send(from_y.at[pl.ds(half, half)], from_y.at[pl.ds(half, half)], base + 8, x_peer)
        send(from_y, from_y, base + 5, c_peer)

    def gather_diag(g):
        base = g * PER_GROUP
        far = block(g, 1 - x, 1 - y, c)
        arrived(far.at[pl.ds(0, half)], base + 7)
        arrived(far.at[pl.ds(half, half)], base + 8)
        send(far, far, base + 6, c_peer)

    def compute(g):
        base = g * PER_GROUP
        arrived(block(g, x, y, 1 - c), base + 3)
        arrived(block(g, 1 - x, y, 1 - c), base + 4)
        arrived(block(g, x, 1 - y, 1 - c), base + 5)
        arrived(block(g, 1 - x, 1 - y, 1 - c), base + 6)
        zz = (z + g) % groups
        squares = jnp.zeros((2 * tok, 1), jnp.float32)
        for s in range(4):
            v = rows_all[zz, s].reshape(2 * tok, width).astype(jnp.float32)
            squares = squares + jnp.sum(v * v, axis=1, keepdims=True)
        scale = lax.rsqrt(squares / model_width + EPSILON)
        for s in range(4):
            v = rows_all[zz, s].reshape(2 * tok, width).astype(jnp.float32)
            normed[:, s * width : (s + 1) * width] = (v * scale * gains[s]).astype(jnp.bfloat16)
        columns = [
            jnp.transpose(jnp.broadcast_to(tables[zz * 2 + xx, pl.ds(e, 1), :], (8, tok)))[:, :1]
            for xx in range(2)
        ]
        share = jnp.concatenate(columns, axis=0)
        lhs = normed[...]
        gate_pre = jnp.minimum(
            jnp.dot(lhs, gate_w[...], preferred_element_type=jnp.float32), CLAMP_LIMIT
        )
        up_pre = jnp.clip(
            jnp.dot(lhs, up_w[...], preferred_element_type=jnp.float32), -CLAMP_LIMIT, CLAMP_LIMIT
        )
        activated = (
            (up_pre + 1.0) * gate_pre * jax.nn.sigmoid(SIGMOID_SLOPE * gate_pre) * share
        ).astype(jnp.bfloat16)

        def project(j, cc):
            yy = y if j == 0 else 1 - y
            start = pl.multiple_of((yy * 2 + cc) * width, width)
            value = jnp.dot(
                activated, down_w[:, pl.ds(start, width)], preferred_element_type=jnp.float32
            )
            return value.reshape(2, tok, width)

        for j in range(2):
            pair_out[g, j] = project(j, 1 - c).astype(jnp.bfloat16)
        send(pair_out.at[g], pair_in.at[g], base + 9, c_peer)
        for j in range(2):
            own[g, j] = project(j, c)

    def pair_sum(g, j, xx, start, count):
        rows = pl.ds(start, count)
        return own[g, j, xx, rows, :] + pair_in[g, j, xx, rows, :].astype(jnp.float32)

    low, high = pl.ds(0, half), pl.ds(half, half)

    def reduce_first(g):
        base = g * PER_GROUP
        arrived(pair_in.at[g], base + 9)
        diag_out[g] = pair_sum(g, 1, 1 - x, 0, tok).astype(jnp.bfloat16)
        send(diag_out.at[g, low], diag_x.at[g], base + 10, x_peer)
        send(diag_out.at[g, high], diag_y.at[g], base + 11, y_peer)
        x_out[g, low] = pair_sum(g, 0, 1 - x, 0, half).astype(jnp.bfloat16)
        send(x_out.at[g, low], x_in.at[g, low], base + 12, x_peer)
        y_out[g, high] = pair_sum(g, 1, x, half, half).astype(jnp.bfloat16)
        send(y_out.at[g, high], y_in.at[g, high], base + 13, y_peer)

    def reduce_second(g):
        base = g * PER_GROUP
        arrived(diag_x.at[g], base + 10)
        y_out[g, low] = (
            pair_sum(g, 1, x, 0, half) + diag_x[g].astype(jnp.float32)
        ).astype(jnp.bfloat16)
        send(y_out.at[g, low], y_in.at[g, low], base + 14, y_peer)
        arrived(diag_y.at[g], base + 11)
        x_out[g, high] = (
            pair_sum(g, 0, 1 - x, half, half) + diag_y[g].astype(jnp.float32)
        ).astype(jnp.bfloat16)
        send(x_out.at[g, high], x_in.at[g, high], base + 15, x_peer)

    def reduce_third(g):
        base = g * PER_GROUP
        arrived(x_in.at[g, low], base + 12)
        arrived(y_in.at[g, high], base + 13)
        arrived(y_in.at[g, low], base + 14)
        arrived(x_in.at[g, high], base + 15)
        total = (
            pair_sum(g, 0, x, 0, tok) + x_in[g].astype(jnp.float32) + y_in[g].astype(jnp.float32)
        )
        if g:
            back = groups - g
            z_out[g] = total.astype(jnp.bfloat16)
            send(
                z_out.at[g],
                z_in.at[back],
                back * PER_GROUP + 16,
                device((z + g) % groups, x, y, c),
            )
        else:
            home[...] = total

    order = sorted(range(groups), key=lambda g: min(g, groups - g))

    for g in order[1:]:
        back = groups - g
        send(tokens, block(0, x, y, c), back * PER_GROUP, device((z + g) % groups, x, y, c))
    gather_z(0)
    for (dy, dc), peer in tp_peers.items():
        send(norm_gain, gains.at[t], small + ep_size + dy * 2 + dc, peer)
    for (dz, dx), peer in ep_peers.items():
        send(table, tables.at[e], small + ((groups - dz) % groups) * 2 + dx, peer)

    if groups > 1:
        gather_z(order[1])
    gather_xy(0)
    for i, g in enumerate(order):
        if i + 2 < groups:
            gather_z(order[i + 2])
        if i + 1 < groups:
            gather_xy(order[i + 1])
        gather_diag(g)
        if i == 0:
            for dy, dc in tp_peers:
                arrived(gains.at[t], small + ep_size + dy * 2 + dc)
            for dz, dx in ep_peers:
                arrived(tables.at[e], small + dz * 2 + dx)
            for load in loads:
                load.wait()
        else:
            reduce_first(order[i - 1])
        compute(g)
        if i >= 1:
            reduce_second(order[i - 1])
        if i >= 2:
            reduce_third(order[i - 2])
    reduce_first(order[-1])
    if groups > 1:
        reduce_third(order[-2])
    reduce_second(order[-1])
    reduce_third(order[-1])

    mixture = home[...]
    for g in order[1:]:
        arrived(z_in.at[g], g * PER_GROUP + 16)
        mixture = mixture + z_in[g].astype(jnp.float32)
    partial_squares = jnp.sum(mixture * mixture, axis=1, keepdims=True)
    square_out[...] = jnp.transpose(jnp.broadcast_to(partial_squares, (tok, 128)))[:8]
    squares = square_out[...]
    for (dy, dc), peer in tp_peers.items():
        send(square_out, squares_in.at[dy * 2 + dc], small + ep_size + 4 + dy * 2 + dc, peer)
    for dy, dc in tp_peers:
        arrived(squares_in.at[dy * 2 + dc], small + ep_size + 4 + dy * 2 + dc)
        squares = squares + squares_in[dy * 2 + dc]
    scale = lax.rsqrt(jnp.transpose(squares)[:, :1] / model_width + EPSILON)
    out[...] = (mixture * scale * final_gain[...]).astype(jnp.bfloat16)
    for copy in sent:
        copy.wait_send()


def fused_local(
    ep_size,
    tokens,
    norm_gain,
    expert_ids,
    route_weights,
    gate_proj,
    up_proj,
    down_proj,
    final_gain,
):
    tok, width = tokens.shape
    model_width, hidden = gate_proj.shape[1:]
    groups = ep_size // 2
    half = tok // 2
    bf16, f32 = jnp.bfloat16, jnp.float32
    slots = groups * PER_GROUP + ep_size + 8
    vmem = pl.BlockSpec(memory_space=pltpu.VMEM)
    hbm = pl.BlockSpec(memory_space=pl.ANY)
    return pl.pallas_call(
        functools.partial(fused_kernel, ep_size),
        out_shape=jax.ShapeDtypeStruct((tok, width), bf16),
        in_specs=[vmem] * 4 + [hbm] * 3 + [vmem],
        out_specs=vmem,
        scratch_shapes=[
            pltpu.VMEM((groups, 4, 2, tok, width), bf16),
            pltpu.VMEM((model_width, hidden), bf16),
            pltpu.VMEM((model_width, hidden), bf16),
            pltpu.VMEM((hidden, model_width), bf16),
            pltpu.VMEM((2 * tok, model_width), bf16),
            pltpu.VMEM((4, 1, width), f32),
            pltpu.VMEM((ep_size, tok), f32),
            pltpu.VMEM((ep_size, ep_size, tok), f32),
            pltpu.VMEM((groups, 2, 2, tok, width), f32),
            pltpu.VMEM((groups, 2, 2, tok, width), bf16),
            pltpu.VMEM((groups, 2, 2, tok, width), bf16),
            pltpu.VMEM((groups, tok, width), bf16),
            pltpu.VMEM((groups, tok, width), bf16),
            pltpu.VMEM((groups, tok, width), bf16),
            pltpu.VMEM((groups, tok, width), bf16),
            pltpu.VMEM((groups, half, width), bf16),
            pltpu.VMEM((groups, half, width), bf16),
            pltpu.VMEM((groups, tok, width), bf16),
            pltpu.VMEM((groups, tok, width), bf16),
            pltpu.VMEM((groups, tok, width), bf16),
            pltpu.VMEM((tok, width), f32),
            pltpu.VMEM((8, tok), f32),
            pltpu.VMEM((4, 8, tok), f32),
            pltpu.SemaphoreType.DMA((3,)),
            pltpu.SemaphoreType.DMA((slots,)),
            pltpu.SemaphoreType.DMA((slots,)),
        ],
        compiler_params=pltpu.CompilerParams(
            collective_id=0, has_side_effects=True, vmem_limit_bytes=48 * 1024 * 1024
        ),
    )(
        tokens,
        norm_gain[None, :],
        expert_ids,
        route_weights,
        gate_proj,
        up_proj,
        down_proj,
        final_gain[None, :],
    )


def solution(mesh):
    placed = (
        P("ep", "tp"),
        P("tp"),
        P("ep", None),
        P("ep", None),
        P("ep", None, "tp"),
        P("ep", None, "tp"),
        P("ep", "tp", None),
        P("tp"),
    )
    def step(*args):
        tok_rows, choose_count = args[2].shape
        capacity = min(tok_rows, 2 * tok_rows * choose_count // mesh.shape["ep"])
        if capacity == tok_rows and mesh.shape["tp"] == 4 and mesh.shape["ep"] % 2 == 0:
            return fused_local(mesh.shape["ep"], *args)
        return local(*args)

    return jax.shard_map(
        step, mesh=mesh, in_specs=placed, out_specs=P("ep", "tp"), check_vma=False
    )
```

```python
import functools

import jax
import jax.numpy as jnp
from jax import lax
from jax.experimental import pallas as pl
from jax.experimental.pallas import tpu as pltpu
from jax.sharding import PartitionSpec as P

EPSILON = 1e-05
CLAMP_LIMIT = 7.0
MESH = pl.DeviceIdType.MESH
PER_GROUP = 17
SIGMOID_SLOPE = 1.702


def slot_tables(id_block, gate_block, targets, capacity):
    matches = (id_block[:, :, None] == targets[None, None, :]).astype(jnp.int32)
    per_token = jnp.sum(matches, axis=1)
    earlier = jnp.cumsum(per_token, axis=0) - per_token
    slot_places = lax.broadcasted_iota(jnp.int32, (1, 1, capacity), 2)
    selector = (
        per_token[:, :, None] * (earlier[:, :, None] == slot_places).astype(jnp.int32)
    ).astype(jnp.float32)
    weights = jnp.sum(gate_block[:, :, None] * matches.astype(jnp.float32), axis=1)
    return (selector, weights)


def expert_partial(flat_rows, gate_proj, up_proj, down_proj):
    gate_pre = jnp.minimum(
        jnp.dot(flat_rows, gate_proj[0], preferred_element_type=jnp.float32), CLAMP_LIMIT
    )
    up_pre = jnp.clip(
        jnp.dot(flat_rows, up_proj[0], preferred_element_type=jnp.float32),
        -CLAMP_LIMIT,
        CLAMP_LIMIT,
    )
    activated = ((up_pre + 1.0) * gate_pre * jax.nn.sigmoid(SIGMOID_SLOPE * gate_pre)).astype(
        jnp.bfloat16
    )
    return jnp.dot(activated, down_proj[0], preferred_element_type=jnp.float32)


def local(tokens, norm_gain, expert_ids, route_weights, gate_proj, up_proj, down_proj, final_gain):
    tok_rows, local_width = tokens.shape
    choose_count = expert_ids.shape[1]
    model_width = local_width * lax.axis_size("tp")
    expert_count = lax.axis_size("ep")
    capacity = min(tok_rows, 2 * tok_rows * choose_count // expert_count)
    input_rows = tokens.astype(jnp.float32)
    squares = lax.psum(jnp.sum(input_rows * input_rows, axis=1), "tp")
    normed = (
        input_rows * lax.rsqrt(squares / model_width + EPSILON)[:, None] * norm_gain[None, :]
    ).astype(jnp.bfloat16)
    targets = lax.iota(jnp.int32, expert_count)
    selector, weights = slot_tables(expert_ids, route_weights, targets, capacity)
    picker = selector.astype(jnp.bfloat16)
    outbound = jnp.einsum("tec,td->ecd", picker, normed, preferred_element_type=jnp.float32).astype(
        jnp.bfloat16
    )
    received = lax.all_gather(
        lax.all_to_all(outbound, "ep", split_axis=0, concat_axis=0, tiled=True),
        "tp",
        axis=2,
        tiled=True,
    )
    flat_rows = received.reshape(-1, model_width)
    partial_value = expert_partial(flat_rows, gate_proj, up_proj, down_proj)
    summed = lax.psum_scatter(
        partial_value.astype(jnp.bfloat16), "tp", scatter_dimension=1, tiled=True
    )
    expert_out = summed.reshape(received.shape[0], received.shape[1], local_width)
    returned = lax.all_to_all(expert_out, "ep", split_axis=0, concat_axis=0, tiled=True)
    mixture = jnp.einsum(
        "tec,ecd->td", selector * weights[:, :, None], returned.astype(jnp.float32)
    )
    squares_out = lax.psum(jnp.sum(mixture * mixture, axis=1), "tp")
    return (
        mixture * lax.rsqrt(squares_out / model_width + EPSILON)[:, None] * final_gain[None, :]
    ).astype(jnp.bfloat16)


def stage_plan(groups):
    plan = [("z", 1), ("x", 0), ("z", 2), ("g", 0), ("x", 1), ("d", 0)]
    for i in range(groups):
        plan += [("z", i + 3), ("x", i + 2), ("u", i), ("d", i + 1), ("v", i)]
        plan += [("1", i - 1), ("2", i - 2), ("3", i - 3)]
    last = groups - 1
    plan += [("1", last), ("2", last - 1), ("3", last - 2), ("2", last), ("3", last - 1), ("3", last)]
    return [(kind, place) for kind, place in plan if 0 <= place < groups]


def fused_kernel(
    ep_size,
    tokens_hbm,
    gain_hbm,
    ids_hbm,
    route_hbm,
    gate_hbm,
    up_hbm,
    down_hbm,
    final_hbm,
    out,
    rows_all,
    expert_ids,
    route_weights,
    final_gain,
    gate_w,
    up_w,
    down_w,
    hidden_act,
    gains,
    table,
    tables,
    own,
    pair_out,
    pair_in,
    diag_out,
    x_out,
    y_out,
    z_out,
    diag_x,
    diag_y,
    x_in,
    y_in,
    z_in,
    home,
    square_out,
    squares_in,
    weight_sem,
    send_sem,
    recv_sem,
):
    groups = ep_size // 2
    tok, width = tokens_hbm.shape
    half = tok // 2
    model_width = 4 * width
    e, t = lax.axis_index("ep"), lax.axis_index("tp")
    z, x, y, c = e // 2, e % 2, t // 2, t % 2

    def device(zz, xx, yy, cc):
        return (zz * 2 + xx, yy * 2 + cc)

    x_peer, y_peer, c_peer = device(z, 1 - x, y, c), device(z, x, 1 - y, c), device(z, x, y, 1 - c)
    tp_peers = {(1, 0): y_peer, (0, 1): c_peer, (1, 1): device(z, x, 1 - y, 1 - c)}
    ep_peers = {
        (dz, dx): device((z + dz) % groups, (x + dx) % 2, y, c)
        for dz in range(groups)
        for dx in range(2)
        if dz or dx
    }

    loads = [
        pltpu.make_async_copy(src, dst, weight_sem.at[i])
        for i, (src, dst) in enumerate(
            (
                (tokens_hbm, rows_all.at[z, t, x]),
                (ids_hbm, expert_ids),
                (route_hbm, route_weights),
                (gain_hbm, gains.at[t]),
                (final_hbm, final_gain),
                (gate_hbm.at[0], gate_w),
                (up_hbm.at[0], up_w),
                (down_hbm.at[0], down_w),
            )
        )
    ]
    for load in loads:
        load.start()

    barrier = pltpu.get_barrier_semaphore()
    peers = list(tp_peers.values()) + list(ep_peers.values())
    for peer in peers:
        pl.semaphore_signal(barrier, inc=1, device_id=peer, device_id_type=MESH)

    for load in loads[:4]:
        load.wait()
    experts = lax.broadcasted_iota(jnp.int32, (ep_size, tok), 0)
    dense = jnp.zeros((ep_size, tok), jnp.float32)
    for k in range(expert_ids.shape[0]):
        dense = dense + jnp.where(
            expert_ids[k : k + 1, :] == experts, route_weights[k : k + 1, :], 0.0
        )
    table[...] = dense
    tables[e] = dense
    pl.semaphore_wait(barrier, len(peers))

    sent = []

    def remote(src, dst, slot, peer):
        return pltpu.make_async_remote_copy(
            src_ref=src,
            dst_ref=dst,
            send_sem=send_sem.at[slot],
            recv_sem=recv_sem.at[slot],
            device_id=peer,
            device_id_type=MESH,
        )

    def send(src, dst, slot, peer):
        copy = remote(src, dst, slot, peer)
        copy.start()
        sent.append(copy)

    def arrived(dst, slot):
        remote(dst, dst, slot, c_peer).wait_recv()

    def block(g, xx, yy, cc):
        return rows_all.at[(z + g) % groups, yy * 2 + cc, xx]

    small = groups * PER_GROUP

    def gather_z(g):
        if g:
            arrived(block(g, x, y, c), g * PER_GROUP)
        src = dst = block(g, x, y, c)
        send(src, dst, g * PER_GROUP + 1, x_peer)
        send(src, dst, g * PER_GROUP + 2, y_peer)
        send(src, dst, g * PER_GROUP + 3, c_peer)

    def gather_xy(g):
        base = g * PER_GROUP
        from_x = block(g, 1 - x, y, c)
        arrived(from_x, base + 1)
        send(from_x.at[pl.ds(0, half)], from_x.at[pl.ds(0, half)], base + 7, y_peer)
        send(from_x, from_x, base + 4, c_peer)
        from_y = block(g, x, 1 - y, c)
        arrived(from_y, base + 2)
        send(from_y.at[pl.ds(half, half)], from_y.at[pl.ds(half, half)], base + 8, x_peer)
        send(from_y, from_y, base + 5, c_peer)

    def gather_diag(g):
        base = g * PER_GROUP
        far = block(g, 1 - x, 1 - y, c)
        arrived(far.at[pl.ds(0, half)], base + 7)
        arrived(far.at[pl.ds(half, half)], base + 8)
        send(far, far, base + 6, c_peer)

    def expand(g):
        base = g * PER_GROUP
        arrived(block(g, x, y, 1 - c), base + 3)
        arrived(block(g, 1 - x, y, 1 - c), base + 4)
        arrived(block(g, x, 1 - y, 1 - c), base + 5)
        arrived(block(g, 1 - x, 1 - y, 1 - c), base + 6)
        zz = (z + g) % groups
        slices = [rows_all[zz, s].reshape(2 * tok, width) for s in range(4)]
        squares = jnp.zeros((2 * tok, width), jnp.float32)
        for v in slices:
            v = v.astype(jnp.float32)
            squares = squares + v * v
        scale = lax.rsqrt(jnp.sum(squares, axis=1, keepdims=True) / model_width + EPSILON)
        columns = [
            jnp.transpose(jnp.broadcast_to(tables[zz * 2 + xx, pl.ds(e, 1), :], (8, tok)))[:, :1]
            for xx in range(2)
        ]
        share = jnp.concatenate(columns, axis=0)
        lhs = jnp.concatenate(slices, axis=1)
        gate_pre = jnp.minimum(
            jnp.dot(lhs, gate_w[...], preferred_element_type=jnp.float32) * scale, CLAMP_LIMIT
        )
        up_pre = jnp.clip(
            jnp.dot(lhs, up_w[...], preferred_element_type=jnp.float32) * scale,
            -CLAMP_LIMIT,
            CLAMP_LIMIT,
        )
        hidden_act[g] = (
            (up_pre + 1.0) * gate_pre * jax.nn.sigmoid(SIGMOID_SLOPE * gate_pre) * share
        ).astype(jnp.bfloat16)

    def contract(g):
        base = g * PER_GROUP
        activated = hidden_act[g]

        def project(j, cc):
            yy = y if j == 0 else 1 - y
            start = pl.multiple_of((yy * 2 + cc) * width, width)
            value = jnp.dot(
                activated, down_w[:, pl.ds(start, width)], preferred_element_type=jnp.float32
            )
            return value.reshape(2, tok, width)

        for j in range(2):
            pair_out[g, j] = project(j, 1 - c).astype(jnp.bfloat16)
        send(pair_out.at[g], pair_in.at[g], base + 9, c_peer)
        for j in range(2):
            own[g, j] = project(j, c)

    def pair_sum(g, j, xx, start, count):
        rows = pl.ds(start, count)
        return own[g, j, xx, rows, :] + pair_in[g, j, xx, rows, :].astype(jnp.float32)

    low, high = pl.ds(0, half), pl.ds(half, half)

    def reduce_first(g):
        base = g * PER_GROUP
        arrived(pair_in.at[g], base + 9)
        diag_out[g] = pair_sum(g, 1, 1 - x, 0, tok).astype(jnp.bfloat16)
        send(diag_out.at[g, low], diag_x.at[g], base + 10, x_peer)
        send(diag_out.at[g, high], diag_y.at[g], base + 11, y_peer)
        x_out[g, low] = pair_sum(g, 0, 1 - x, 0, half).astype(jnp.bfloat16)
        send(x_out.at[g, low], x_in.at[g, low], base + 12, x_peer)
        y_out[g, high] = pair_sum(g, 1, x, half, half).astype(jnp.bfloat16)
        send(y_out.at[g, high], y_in.at[g, high], base + 13, y_peer)

    def reduce_second(g):
        base = g * PER_GROUP
        arrived(diag_x.at[g], base + 10)
        y_out[g, low] = (
            pair_sum(g, 1, x, 0, half) + diag_x[g].astype(jnp.float32)
        ).astype(jnp.bfloat16)
        send(y_out.at[g, low], y_in.at[g, low], base + 14, y_peer)
        arrived(diag_y.at[g], base + 11)
        x_out[g, high] = (
            pair_sum(g, 0, 1 - x, half, half) + diag_y[g].astype(jnp.float32)
        ).astype(jnp.bfloat16)
        send(x_out.at[g, high], x_in.at[g, high], base + 15, x_peer)

    def reduce_third(g):
        base = g * PER_GROUP
        arrived(x_in.at[g, low], base + 12)
        arrived(y_in.at[g, high], base + 13)
        arrived(y_in.at[g, low], base + 14)
        arrived(x_in.at[g, high], base + 15)
        total = (
            pair_sum(g, 0, x, 0, tok) + x_in[g].astype(jnp.float32) + y_in[g].astype(jnp.float32)
        )
        if g:
            back = groups - g
            z_out[g] = total.astype(jnp.bfloat16)
            send(
                z_out.at[g],
                z_in.at[back],
                back * PER_GROUP + 16,
                device((z + g) % groups, x, y, c),
            )
        else:
            home[...] = total

    order = sorted(range(groups), key=lambda g: min(g, groups - g))

    for g in order[1:]:
        back = groups - g
        send(block(0, x, y, c), block(0, x, y, c), back * PER_GROUP, device((z + g) % groups, x, y, c))
    gather_z(0)
    for (dy, dc), peer in tp_peers.items():
        send(gains.at[t], gains.at[t], small + ep_size + dy * 2 + dc, peer)
    for (dz, dx), peer in ep_peers.items():
        send(table, tables.at[e], small + ((groups - dz) % groups) * 2 + dx, peer)

    def settle():
        for dy, dc in tp_peers:
            arrived(gains.at[t], small + ep_size + dy * 2 + dc)
        for dz, dx in ep_peers:
            arrived(tables.at[e], small + dz * 2 + dx)
        for load in loads[4:]:
            load.wait()
        for s in range(4):
            gain = jnp.transpose(jnp.broadcast_to(gains[s], (8, width)))[:, :1]
            for w in (gate_w, up_w):
                part = w[s * width : (s + 1) * width, :].astype(jnp.float32)
                w[s * width : (s + 1) * width, :] = (part * gain).astype(jnp.bfloat16)

    steps = {
        "z": gather_z,
        "x": gather_xy,
        "d": gather_diag,
        "u": expand,
        "v": contract,
        "1": reduce_first,
        "2": reduce_second,
        "3": reduce_third,
    }
    for kind, place in stage_plan(groups):
        if kind == "g":
            settle()
        else:
            steps[kind](order[place])

    mixture = home[...]
    for g in order[1:]:
        arrived(z_in.at[g], g * PER_GROUP + 16)
        mixture = mixture + z_in[g].astype(jnp.float32)
    partial_squares = jnp.sum(mixture * mixture, axis=1, keepdims=True)
    square_out[...] = jnp.transpose(jnp.broadcast_to(partial_squares, (tok, 128)))[:8]
    squares = square_out[...]
    for (dy, dc), peer in tp_peers.items():
        send(square_out, squares_in.at[dy * 2 + dc], small + ep_size + 4 + dy * 2 + dc, peer)
    for dy, dc in tp_peers:
        arrived(squares_in.at[dy * 2 + dc], small + ep_size + 4 + dy * 2 + dc)
        squares = squares + squares_in[dy * 2 + dc]
    scale = lax.rsqrt(jnp.transpose(squares)[:, :1] / model_width + EPSILON)
    out[...] = (mixture * scale * final_gain[...]).astype(jnp.bfloat16)
    for copy in sent:
        copy.wait_send()


def fused_local(
    ep_size,
    tokens,
    norm_gain,
    expert_ids,
    route_weights,
    gate_proj,
    up_proj,
    down_proj,
    final_gain,
):
    tok, width = tokens.shape
    model_width, hidden = gate_proj.shape[1:]
    groups = ep_size // 2
    half = tok // 2
    bf16, f32 = jnp.bfloat16, jnp.float32
    slots = groups * PER_GROUP + ep_size + 8
    vmem = pl.BlockSpec(memory_space=pltpu.VMEM)
    hbm = pl.BlockSpec(memory_space=pltpu.HBM)
    return pl.pallas_call(
        functools.partial(fused_kernel, ep_size),
        out_shape=jax.ShapeDtypeStruct((tok, width), bf16),
        in_specs=[hbm] * 8,
        out_specs=vmem,
        scratch_shapes=[
            pltpu.VMEM((groups, 4, 2, tok, width), bf16),
            pltpu.VMEM((expert_ids.shape[1], tok), jnp.int32),
            pltpu.VMEM((expert_ids.shape[1], tok), f32),
            pltpu.VMEM((1, width), f32),
            pltpu.VMEM((model_width, hidden), bf16),
            pltpu.VMEM((model_width, hidden), bf16),
            pltpu.VMEM((hidden, model_width), bf16),
            pltpu.VMEM((groups, 2 * tok, hidden), bf16),
            pltpu.VMEM((4, 1, width), f32),
            pltpu.VMEM((ep_size, tok), f32),
            pltpu.VMEM((ep_size, ep_size, tok), f32),
            pltpu.VMEM((groups, 2, 2, tok, width), f32),
            pltpu.VMEM((groups, 2, 2, tok, width), bf16),
            pltpu.VMEM((groups, 2, 2, tok, width), bf16),
            pltpu.VMEM((groups, tok, width), bf16),
            pltpu.VMEM((groups, tok, width), bf16),
            pltpu.VMEM((groups, tok, width), bf16),
            pltpu.VMEM((groups, tok, width), bf16),
            pltpu.VMEM((groups, half, width), bf16),
            pltpu.VMEM((groups, half, width), bf16),
            pltpu.VMEM((groups, tok, width), bf16),
            pltpu.VMEM((groups, tok, width), bf16),
            pltpu.VMEM((groups, tok, width), bf16),
            pltpu.VMEM((tok, width), f32),
            pltpu.VMEM((8, tok), f32),
            pltpu.VMEM((4, 8, tok), f32),
            pltpu.SemaphoreType.DMA((8,)),
            pltpu.SemaphoreType.DMA((slots,)),
            pltpu.SemaphoreType.DMA((slots,)),
        ],
        compiler_params=pltpu.CompilerParams(
            collective_id=0, has_side_effects=True, vmem_limit_bytes=67043328
        ),
    )(
        tokens,
        norm_gain[None, :],
        expert_ids.T,
        route_weights.T,
        gate_proj,
        up_proj,
        down_proj,
        final_gain[None, :],
    )


def solution(mesh):
    placed = (
        P("ep", "tp"),
        P("tp"),
        P("ep", None),
        P("ep", None),
        P("ep", None, "tp"),
        P("ep", None, "tp"),
        P("ep", "tp", None),
        P("tp"),
    )
    def step(*args):
        tok_rows, choose_count = args[2].shape
        capacity = min(tok_rows, 2 * tok_rows * choose_count // mesh.shape["ep"])
        if capacity == tok_rows and mesh.shape["tp"] == 4 and mesh.shape["ep"] % 2 == 0:
            return fused_local(mesh.shape["ep"], *args)
        return local(*args)

    return jax.shard_map(
        step, mesh=mesh, in_specs=placed, out_specs=P("ep", "tp"), check_vma=False
    )
```
